32 devices in a mesh: sp: 8 (over z, x), tp: 4 (over y, core).
Axes of the slice: x: 2, y: 2, z: 4, core: 2. Of those that a mesh axis runs over, the one named last changes fastest.
Arguments:
- tokens: bfloat16 [2, 128, 1024], P(None, 'sp', 'tp'), may hold values from -6 to 6
- in_weight: bfloat16 [3, 1024, 2048], P(None, 'sp', 'tp'), may hold values from -0.1875 to 0.1875
- gate_weight: bfloat16 [3, 1024, 2048], P(None, 'sp', 'tp'), may hold values from -0.1875 to 0.1875
- out_weight: bfloat16 [3, 2048, 1024], P(None, 'tp', 'sp'), may hold values from -0.25 to 0.25
- recur_weight: bfloat16 [3, 2, 16, 128, 128], P(None, None, 'tp'), may hold values from -0.5 to 0.5
- input_weight: bfloat16 [3, 2, 16, 128, 128], P(None, None, 'tp'), may hold values from -0.5 to 0.5
- conv_taps: bfloat16 [3, 4, 2048], P(None, None, 'tp'), may hold values from -3 to 3
- decay_rate: float32 [3, 2, 2048], P(None, None, 'tp'), may hold values from 0.02 to 0.25
- norm_gain: float32 [3, 1024], replicated, may hold values from 0.5 to 1.5
Outputs:
- mixed_out: bfloat16 [2, 128, 1024], P(None, 'sp', 'tp')
The draws below stay inside these ranges and needn't reach their ends.
All inputs are finite; a program needn't handle non-finite values.
Results may differ from the reference program's by a relative error of at most 0.04.
Values may be sent and summed in bfloat16 or wider, within the bound.
A program may use at most 64 MiB of HBM per device.

```python
import math
import jax
import jax.numpy as jnp
from jax import lax

D = 1024
HEADS = 16
HEAD_DIM = 128
CONV_WIDTH = 4
LAYERS = 3
BATCH = 2
WIDTH = 2048
SEQ = 128


def steps_of(stream_key, shape, shards, least, largest):
    level = 1.0
    for dim, parts in shards:
        heights = jax.random.uniform(jax.random.fold_in(jax.random.fold_in(stream_key, 6), dim), (parts,), jnp.float32, least / len(shards), largest / len(shards))
        level = level * jnp.repeat(jnp.exp(heights), shape[dim] // parts).reshape((-1,) + (1,) * (len(shape) - 1 - dim))
    return level


def centred(key, shape, width, most, split=(), dtype=jnp.bfloat16):
    level = steps_of(key, shape, split, -0.22, 0.18) if split else 1.0
    array = jax.random.normal(key, shape, jnp.float32) * width * level
    return jnp.minimum(jnp.maximum(array, -most), most).astype(dtype)


def setup_inputs(seed: int = 0) -> dict:
    key_of = jax.random.split(jax.random.key(seed), 10)
    tokens = centred(key_of[0], (BATCH, SEQ, D), 1.0, 6.0, ((1, 8), (2, 4)))
    in_weight = centred(key_of[1], (LAYERS, D, WIDTH), D ** -0.5, 0.1875, ((1, 8), (2, 4)))
    gate_weight = centred(key_of[2], (LAYERS, D, WIDTH), D ** -0.5, 0.1875, ((1, 8), (2, 4)))
    out_weight = centred(key_of[3], (LAYERS, WIDTH, D), (WIDTH // 4) ** -0.5, 0.25, ((1, 4), (2, 8)))
    recur_weight = centred(key_of[4], (LAYERS, 2, HEADS, HEAD_DIM, HEAD_DIM), HEAD_DIM ** -0.5, 0.5, ((2, 4),))
    input_weight = centred(key_of[5], (LAYERS, 2, HEADS, HEAD_DIM, HEAD_DIM), HEAD_DIM ** -0.5, 0.5, ((2, 4),))
    conv_taps = centred(key_of[6], (LAYERS, CONV_WIDTH, WIDTH), CONV_WIDTH ** -0.5, 3.0, ((2, 4),))
    decay_rate = jnp.clip(jnp.exp(math.log(0.25) - 2.5257287 * jax.random.uniform(key_of[7], (LAYERS, 2, WIDTH), jnp.float32) ** steps_of(key_of[7], (LAYERS, 2, WIDTH), ((2, 4),), -0.2, 0.2)), 0.02, 0.25)
    norm_gain = jnp.clip(1.0 + 0.1 * jax.random.normal(key_of[8], (LAYERS, D), jnp.float32), 0.5, 1.5)
    return dict(tokens=tokens, in_weight=in_weight, gate_weight=gate_weight, out_weight=out_weight, recur_weight=recur_weight, input_weight=input_weight, conv_taps=conv_taps, decay_rate=decay_rate, norm_gain=norm_gain)


epsilon = 1e-06
gate_power = 8.0

def combine(earlier, later_pair):
    first_decay, first_drive = earlier
    second_decay, second_drive = later_pair
    return (first_decay * second_decay, second_decay * first_drive + second_drive)

def reference(tokens, in_weight, gate_weight, out_weight, recur_weight, input_weight, conv_taps, decay_rate, norm_gain):
    batch_size, seq_len, _ = tokens.shape
    state = tokens
    for layer_index in range(LAYERS):
        flat_rows = state.reshape(batch_size * seq_len, D).astype(jnp.float32)
        scale_rows = lax.rsqrt(lax.optimization_barrier(jnp.mean(flat_rows * flat_rows, axis=-1, keepdims=True)) + epsilon)
        normed = (flat_rows * scale_rows * norm_gain[layer_index]).astype(jnp.bfloat16)
        branch = jnp.dot(normed, in_weight[layer_index], preferred_element_type=jnp.float32).astype(jnp.bfloat16)
        gate_branch = jnp.dot(normed, gate_weight[layer_index], preferred_element_type=jnp.float32).astype(jnp.bfloat16)
        branch = branch.reshape(batch_size, seq_len, WIDTH)
        gate_branch = gate_branch.reshape(batch_size, seq_len, WIDTH)
        padded = jnp.pad(branch.astype(jnp.float32), ((0, 0), (2, 1), (0, 0)))
        tap_values = conv_taps[layer_index].astype(jnp.float32)
        conv_out = padded[:, 0:seq_len] * tap_values[0]
        for tap_index in range(1, CONV_WIDTH):
            conv_out = conv_out + padded[:, tap_index:tap_index + seq_len] * tap_values[tap_index]
        conv_out = conv_out.astype(jnp.bfloat16)
        conv_float = conv_out.astype(jnp.float32)
        blocks = conv_float.reshape(batch_size, seq_len, HEADS, HEAD_DIM)
        hidden_sum = jnp.zeros((batch_size, seq_len, WIDTH), jnp.float32)
        for direction in range(2):
            recur_gate = jax.nn.sigmoid(jnp.einsum('bthd,hde->bthe', blocks, recur_weight[layer_index, direction].astype(jnp.float32))).reshape(batch_size, seq_len, WIDTH)
            input_gate = jax.nn.sigmoid(jnp.einsum('bthd,hde->bthe', blocks, input_weight[layer_index, direction].astype(jnp.float32))).reshape(batch_size, seq_len, WIDTH)
            log_decay = -gate_power * recur_gate * decay_rate[layer_index, direction] / SEQ
            decay_step = jnp.exp(log_decay)
            driven = jnp.sqrt(-jnp.expm1(2.0 * log_decay)) * input_gate * conv_float
            cum_decay, cum_drive = lax.associative_scan(combine, (decay_step, driven), axis=1, reverse=direction == 1)
            hidden_sum = hidden_sum + cum_drive
        mixed_rows = (hidden_sum * jax.nn.silu(gate_branch.astype(jnp.float32))).astype(jnp.bfloat16)
        mixed_rows = mixed_rows.reshape(batch_size * seq_len, WIDTH)
        result = jnp.dot(mixed_rows, out_weight[layer_index], preferred_element_type=jnp.float32).astype(jnp.bfloat16)
        state = result.reshape(batch_size, seq_len, D)
    return state
```

```python
import functools

import jax
import jax.numpy as jnp
from jax import lax
from jax.experimental import pallas as pl
from jax.experimental.pallas import tpu as pltpu
from jax.sharding import PartitionSpec as P

LAYERS = 3


epsilon = 1e-06
gate_power = 8.0


def extended(array, sides, width, wrap):
    for axis, dim in sides:
        size, length = lax.axis_size(axis), array.shape[dim]
        up = [(i, (i + 1) % size) for i in range(size if wrap else size - 1)]
        down = [(j, i) for i, j in up]
        last = lax.slice_in_dim(array, length - width, length, axis=dim)
        initial = lax.slice_in_dim(array, 0, width, axis=dim)
        before = lax.ppermute(last, axis, up)
        after = lax.ppermute(initial, axis, down)
        array = jnp.concatenate([before, array, after], axis=dim)
    return array


def carried_in(value, axis, join, neutral, backward):
    count, mine = lax.axis_size(axis), lax.axis_index(axis)
    pieces = jax.tree.map(lambda part: lax.all_gather(part, axis), value)
    if backward:
        pieces = jax.tree.map(lambda part: part[::-1], pieces)
        mine = count - 1 - mine
    subtotal = jax.tree.map(
        lambda part, zero: jnp.full_like(part, 0) + jnp.asarray(zero, part.dtype), value, neutral
    )

    def hop(position, subtotal):
        longer = join(subtotal, jax.tree.map(lambda part: part[position], pieces))
        return jax.tree.map(lambda new, old: jnp.where(position < mine, new, old), longer, subtotal)

    return lax.fori_loop(0, count - 1, hop, subtotal)


def combine(earlier, later_pair):
    first_decay, first_drive = earlier
    second_decay, second_drive = later_pair
    return (first_decay * second_decay, second_decay * first_drive + second_drive)


def body(
    tokens,
    in_weight,
    gate_weight,
    out_weight,
    recur_weight,
    input_weight,
    conv_taps,
    decay_rate,
    norm_gain,
):
    batch_size, tok_rows, _ = tokens.shape
    seq_len = tok_rows * lax.axis_size("sp")
    chan_width = in_weight.shape[2]
    in_whole, gate_whole = (
        lax.all_gather(in_weight, "sp", axis=1, tiled=True),
        lax.all_gather(gate_weight, "sp", axis=1, tiled=True),
    )
    out_whole = lax.all_gather(out_weight, "sp", axis=2, tiled=True)
    state = tokens
    for layer_index in range(LAYERS):
        gathered = lax.all_gather(state, "tp", axis=2, tiled=True)
        flat_rows = gathered.reshape(batch_size * tok_rows, -1).astype(jnp.float32)
        scale_rows = lax.rsqrt(jnp.mean(flat_rows * flat_rows, axis=-1, keepdims=True) + epsilon)
        normed = (flat_rows * scale_rows * norm_gain[layer_index]).astype(jnp.bfloat16)
        branch = jnp.dot(normed, in_whole[layer_index], preferred_element_type=jnp.float32)
        gate_branch = jnp.dot(normed, gate_whole[layer_index], preferred_element_type=jnp.float32)
        branch = branch.astype(jnp.bfloat16).reshape(batch_size, tok_rows, chan_width)
        gate_branch = gate_branch.astype(jnp.bfloat16).reshape(batch_size, tok_rows, chan_width)
        padded = extended(branch, (("sp", 1),), 2, False)
        tap_values = conv_taps[layer_index].astype(jnp.float32)
        conv_out = padded[:, 0:tok_rows].astype(jnp.float32) * tap_values[0]
        for tap_index in range(1, tap_values.shape[0]):
            conv_out = (
                conv_out
                + padded[:, tap_index : tap_index + tok_rows].astype(jnp.float32)
                * tap_values[tap_index]
            )
        conv_out = conv_out.astype(jnp.bfloat16)
        conv_float = conv_out.astype(jnp.float32)
        recur_full = recur_weight[layer_index]
        input_full = input_weight[layer_index]
        heads_local = recur_full.shape[1]
        head_dim = recur_full.shape[2]
        blocks = conv_out.reshape(batch_size, tok_rows, heads_local, head_dim)
        hidden_sum = jnp.zeros((batch_size, tok_rows, chan_width), jnp.float32)
        identity = (
            jnp.ones((batch_size, chan_width), jnp.float32),
            jnp.zeros((batch_size, chan_width), jnp.float32),
        )
        for direction in range(2):
            recur_gate = jax.nn.sigmoid(
                jnp.einsum(
                    "bthd,hde->bthe",
                    blocks,
                    recur_full[direction],
                    preferred_element_type=jnp.float32,
                )
            ).reshape(batch_size, tok_rows, chan_width)
            input_gate = jax.nn.sigmoid(
                jnp.einsum(
                    "bthd,hde->bthe",
                    blocks,
                    input_full[direction],
                    preferred_element_type=jnp.float32,
                )
            ).reshape(batch_size, tok_rows, chan_width)
            log_decay = -gate_power * recur_gate * decay_rate[layer_index, direction] / seq_len
            decay_step = jnp.exp(log_decay)
            driven = jnp.sqrt(-jnp.expm1(2.0 * log_decay)) * input_gate * conv_float
            backward = direction == 1
            cum_decay, cum_drive = lax.associative_scan(
                combine, (decay_step, driven), axis=1, reverse=backward
            )
            if backward:
                totals = (cum_decay[:, 0], cum_drive[:, 0])
                incoming = carried_in(totals, "sp", combine, identity, True)
            else:
                totals = (cum_decay[:, -1], cum_drive[:, -1])
                incoming = carried_in(totals, "sp", combine, identity, False)
            hidden_sum = hidden_sum + (cum_decay * incoming[1][:, None, :] + cum_drive)
        mixed_rows = (hidden_sum * jax.nn.silu(gate_branch.astype(jnp.float32))).astype(
            jnp.bfloat16
        )
        mixed_rows = mixed_rows.reshape(batch_size * tok_rows, chan_width)
        partial_terms = jnp.dot(
            mixed_rows, out_whole[layer_index], preferred_element_type=jnp.float32
        )
        shard_sum = lax.psum_scatter(
            partial_terms.astype(jnp.bfloat16), "tp", scatter_dimension=1, tiled=True
        ).astype(jnp.float32)
        state = shard_sum.astype(jnp.bfloat16).reshape(batch_size, tok_rows, -1)
    return state


MESH = pl.DeviceIdType.MESH


def shifted(value, distance, fill, backward):
    rows = value.shape[0]
    row = lax.broadcasted_iota(jnp.int32, value.shape, 0)
    if backward:
        moved = pltpu.roll(value, rows - distance, axis=0)
        return jnp.where(row < rows - distance, moved, fill)
    moved = pltpu.roll(value, distance, axis=0)
    return jnp.where(row >= distance, moved, fill)


def scan_rows(decay, drive, backward):
    distance = 1
    while distance < decay.shape[0]:
        drive = drive + decay * shifted(drive, distance, 0.0, backward)
        if 2 * distance < decay.shape[0]:
            decay = decay * shifted(decay, distance, 1.0, backward)
        distance *= 2
    return drive


def one_minus_exp(value):
    grown = jnp.exp(value)
    safe = jnp.where(grown == 1.0, 0.5, grown)
    return jnp.where(grown == 1.0, -value, (1.0 - safe) * value / jnp.log(safe))


def fused_kernel(
    sizes,
    tok_ref,
    in_ref,
    gate_ref,
    out_w_ref,
    recur_ref,
    input_ref,
    taps_ref,
    rate_ref,
    gain_ref,
    out_ref,
    weights,
    out_weights,
    states,
    mixed,
    terms,
    parts,
    arrived,
    last,
    final,
    w_send,
    w_recv,
    wx_send,
    wx_recv,
    o_send,
    o_recv,
    tok_send,
    tok_recv,
    sz_send,
    sz_recv,
    st_send,
    st_recv,
    mx_send,
    mx_recv,
    p_send,
    p_recv,
    f_send,
    f_recv,
):
    batch, groups, shards, head, seq_len = sizes
    layers = in_ref.shape[0]
    span = tok_ref.shape[1]
    chunk = seq_len // shards
    me, t = lax.axis_index("sp"), lax.axis_index("tp")
    z, x = me // batch, me % batch
    other = batch - 1 - x
    z_at = lambda d: (z + d) % groups
    t_at = lambda d: (t + d) % shards
    device = lambda zz, xx, tt: (zz * batch + xx, tt)
    lanes = lambda index: pl.ds(pl.multiple_of(index * head, head), head)
    pending = []

    def send(src, dst, send_sem, recv_sem, target):
        copy = pltpu.make_async_remote_copy(
            src_ref=src,
            dst_ref=dst,
            send_sem=send_sem,
            recv_sem=recv_sem,
            device_id=target,
            device_id_type=MESH,
        )
        copy.start()
        pending.append(copy)

    def receive(dst, send_sem, recv_sem):
        pltpu.make_async_remote_copy(
            src_ref=dst,
            dst_ref=dst,
            send_sem=send_sem,
            recv_sem=recv_sem,
            device_id=(me, t),
            device_id_type=MESH,
        ).wait_recv()

    barrier = pltpu.get_barrier_semaphore()

    def greet(target):
        pl.semaphore_signal(barrier, inc=1, device_id=target, device_id_type=MESH)

    greet(device(z, other, t))
    for d in range(1, groups):
        greet(device(z_at(d), x, t))
    for d in range(1, shards):
        greet(device(z, x, t_at(d)))

    @pl.when(z != t)
    def _():
        for xx in range(batch):
            greet(device(t, xx, z))

    for layer in range(layers):
        weights[layer, me, :, 0:head] = in_ref[layer, :, lanes(z)]
        weights[layer, me, :, head : 2 * head] = gate_ref[layer, :, lanes(z)]
        out_weights[layer, :, lanes(x)] = out_w_ref[layer]
    rows_here = pl.ds(pl.multiple_of(x * span, span), span)
    states[0, t, z, rows_here, :] = tok_ref[x]

    @pl.when(z == t)
    def _():
        pl.semaphore_wait(barrier, groups + shards - 1)

    @pl.when(z != t)
    def _():
        pl.semaphore_wait(barrier, groups + shards - 1 + batch)

    def send_weights(layer):
        for d in range(1, groups):
            for which, ref in enumerate((in_ref, gate_ref)):
                send(
                    ref.at[layer, :, lanes(z_at(d))],
                    weights.at[layer, me, :, which * head : (which + 1) * head],
                    w_send.at[layer, d, which],
                    w_recv.at[layer, d, which],
                    device(z_at(d), x, t),
                )

    def send_own(layer):
        for which, ref in enumerate((in_ref, gate_ref)):
            send(
                ref.at[layer, :, lanes(z)],
                weights.at[layer, me, :, which * head : (which + 1) * head],
                wx_send.at[layer, 0, which],
                wx_recv.at[layer, 0, which],
                device(z, other, t),
            )

    def send_out(layer):
        send(
            out_w_ref.at[layer],
            out_weights.at[layer, :, lanes(x)],
            o_send.at[layer],
            o_recv.at[layer],
            device(z, other, t),
        )

    def forward_weights(layer):
        for d in range(1, groups):
            block = z_at(groups - d) * batch + x
            for which in range(2):
                view = weights.at[layer, block, :, which * head : (which + 1) * head]
                receive(view, w_send.at[layer, d, which], w_recv.at[layer, d, which])
                send(
                    view,
                    view,
                    wx_send.at[layer, d, which],
                    wx_recv.at[layer, d, which],
                    device(z, other, t),
                )

    def await_weights(layer):
        for d in range(groups):
            block = z_at(groups - d) * batch + other
            for which in range(2):
                view = weights.at[layer, block, :, which * head : (which + 1) * head]
                receive(view, wx_send.at[layer, d, which], wx_recv.at[layer, d, which])

    def spread_start(level, slot):
        here = states.at[(level, *slot(z, t))]
        for d in range(1, groups):
            send(here, here, sz_send.at[level, d], sz_recv.at[level, d], device(z_at(d), x, t))
        for d in range(1, shards):
            send(
                here, here, st_send.at[level, 0, d], st_recv.at[level, 0, d], device(z, x, t_at(d))
            )

    def spread_forward(level, slot):
        for e in range(1, groups):
            view = states.at[(level, *slot(z_at(groups - e), t))]
            receive(view, sz_send.at[level, e], sz_recv.at[level, e])
            for d in range(1, shards):
                send(
                    view,
                    view,
                    st_send.at[level, e, d],
                    st_recv.at[level, e, d],
                    device(z, x, t_at(d)),
                )

    def spread_finish(level, slot):
        for e in range(groups):
            for d in range(1, shards):
                view = states.at[(level, *slot(z_at(groups - e), t_at(shards - d)))]
                receive(view, st_send.at[level, e, d], st_recv.at[level, e, d])

    by_rows = lambda zz, tt: (tt, zz)
    by_columns = lambda zz, tt: (zz, tt)

    landing = states.at[0, t, z, rows_here, :]
    send(tok_ref.at[other], landing, tok_send.at[0], tok_recv.at[0], device(z, other, t))
    send_weights(0)
    send_own(0)
    rows_there = pl.ds(pl.multiple_of(other * span, span), span)
    receive(states.at[0, t, z, rows_there, :], tok_send.at[0], tok_recv.at[0])
    spread_start(0, by_rows)
    send_out(0)
    spread_forward(0, by_rows)
    forward_weights(0)
    if layers > 1:
        send_weights(1)
    spread_finish(0, by_rows)

    for layer in range(layers):
        await_weights(layer)
        depth = states.shape[-1]
        pieces = [
            states[layer, a].reshape(seq_len, depth).astype(jnp.float32) for a in range(groups)
        ]
        squares = sum(jnp.sum(piece * piece, axis=-1, keepdims=True) for piece in pieces)
        scale_rows = lax.rsqrt(squares / (groups * depth) + epsilon)
        gain = gain_ref[layer : layer + 1, :]
        both = jnp.zeros((seq_len, 2 * head), jnp.float32)
        for a in range(groups):
            normed = (pieces[a] * scale_rows * gain[:, a * depth : (a + 1) * depth]).astype(
                jnp.bfloat16
            )
            block = weights[layer, a * batch : (a + 1) * batch].reshape(depth, 2 * head)
            both = both + jnp.dot(normed, block, preferred_element_type=jnp.float32)
        branch = both[:, :head].astype(jnp.bfloat16).astype(jnp.float32)
        gate_branch = both[:, head:].astype(jnp.bfloat16).astype(jnp.float32)
        taps = taps_ref[layer, :, lanes(z)].astype(jnp.float32)
        count = taps.shape[0]
        conv_out = jnp.zeros_like(branch)
        for k in range(count):
            offset = k - count // 2
            moved = branch if offset == 0 else shifted(branch, abs(offset), 0.0, offset > 0)
            conv_out = conv_out + moved * taps[k : k + 1]
        conv_round = conv_out.astype(jnp.bfloat16)
        conv_float = conv_round.astype(jnp.float32)
        hidden_sum = jnp.zeros_like(branch)
        for direction in range(2):
            recur_gate = jax.nn.sigmoid(
                jnp.dot(
                    conv_round, recur_ref[layer, direction, z], preferred_element_type=jnp.float32
                )
            )
            input_gate = jax.nn.sigmoid(
                jnp.dot(
                    conv_round, input_ref[layer, direction, z], preferred_element_type=jnp.float32
                )
            )
            rate = rate_ref[layer, direction : direction + 1, lanes(z)]
            log_decay = recur_gate * (rate * (-gate_power / seq_len))
            decay_step = jnp.exp(log_decay)
            driven = jnp.sqrt(one_minus_exp(2.0 * log_decay)) * input_gate * conv_float
            hidden_sum = hidden_sum + scan_rows(decay_step, driven, direction == 1)
        mixed[layer, z] = (hidden_sum * gate_branch * jax.nn.sigmoid(gate_branch)).astype(
            jnp.bfloat16
        )
        for d in range(1, groups):
            here = mixed.at[layer, z]
            send(here, here, mx_send.at[layer, d], mx_recv.at[layer, d], device(z_at(d), x, t))
        if layer + 1 < layers:
            send_own(layer + 1)
            send_out(layer + 1)
            forward_weights(layer + 1)
        receive(out_weights.at[layer, :, lanes(other)], o_send.at[layer], o_recv.at[layer])
        total = jnp.zeros((seq_len, batch * head), jnp.float32)
        for d in range(groups):
            zz = z_at(groups - d)
            if d:
                receive(mixed.at[layer, zz], mx_send.at[layer, d], mx_recv.at[layer, d])
            rows = pl.ds(pl.multiple_of(zz * head, head), head)
            total = total + jnp.dot(
                mixed[layer, zz], out_weights[layer, rows, :], preferred_element_type=jnp.float32
            )
        for tt in range(shards):
            piece = total[tt * chunk : (tt + 1) * chunk]
            terms[tt] = piece
            parts[layer, tt] = piece.astype(jnp.bfloat16)
        for d in range(1, shards):
            send(
                parts.at[layer, t_at(d)],
                arrived.at[layer, d],
                p_send.at[layer, d],
                p_recv.at[layer, d],
                device(z, x, t_at(d)),
            )
        summed = terms[t]
        for d in range(1, shards):
            receive(arrived.at[layer, d], p_send.at[layer, d], p_recv.at[layer, d])
            summed = summed + arrived[layer, d].astype(jnp.float32)
        summed = summed.astype(jnp.bfloat16)
        if layer + 1 < layers:
            states[layer + 1, z, t] = summed
            spread_start(layer + 1, by_columns)
            if layer + 2 < layers:
                send_weights(layer + 2)
            spread_forward(layer + 1, by_columns)
            spread_finish(layer + 1, by_columns)
        else:
            last[...] = summed.reshape(batch, span, summed.shape[-1])

    def final_copy(e):
        return pltpu.make_async_remote_copy(
            src_ref=last.at[x if e == 0 else other],
            dst_ref=final.at[x],
            send_sem=f_send.at[e],
            recv_sem=f_recv.at[e],
            device_id=device(t, x if e == 0 else other, z),
            device_id_type=MESH,
        )

    @pl.when(z != t)
    def _():
        final_copy(0).start()

    @pl.when(z == t)
    def _():
        final[x] = last[x]

    final_copy(1).start()

    @pl.when(z != t)
    def _():
        receive(final.at[x], f_send.at[0], f_recv.at[0])

    receive(final.at[other], f_send.at[1], f_recv.at[1])
    out_ref[...] = final[...]

    for copy in pending:
        copy.wait_send()

    @pl.when(z != t)
    def _():
        final_copy(0).wait_send()

    final_copy(1).wait_send()


def fused(batch, groups, shards, *args):
    tokens, in_weight, _, out_weight = args[:4]
    layers, rows, width = in_weight.shape
    span, features = tokens.shape[1:]
    head = width // groups
    seq_len = span * batch * groups
    chunk = seq_len // shards
    bf16, f32 = jnp.bfloat16, jnp.float32
    dma = pltpu.SemaphoreType.DMA
    pairs = [
        (layers, groups, 2),
        (layers, groups, 2),
        (layers,),
        (1,),
        (layers, groups),
        (layers, groups, shards),
        (layers, groups),
        (layers, shards),
        (2,),
    ]
    return pl.pallas_call(
        functools.partial(fused_kernel, (batch, groups, shards, head, seq_len)),
        out_shape=jax.ShapeDtypeStruct(tokens.shape, tokens.dtype),
        in_specs=[pl.BlockSpec(memory_space=pltpu.VMEM)] * len(args),
        out_specs=pl.BlockSpec(memory_space=pltpu.VMEM),
        scratch_shapes=[
            pltpu.VMEM((layers, batch * groups, rows, 2 * head), bf16),
            pltpu.VMEM((layers, width, batch * rows), bf16),
            pltpu.VMEM((layers, groups, shards, chunk, features), bf16),
            pltpu.VMEM((layers, groups, seq_len, head), bf16),
            pltpu.VMEM((shards, chunk, batch * rows), f32),
            pltpu.VMEM((layers, shards, chunk, batch * rows), bf16),
            pltpu.VMEM((layers, shards, chunk, batch * rows), bf16),
            pltpu.VMEM((batch, span, batch * rows), bf16),
            pltpu.VMEM((batch, span, features), bf16),
        ]
        + [dma(shape) for shape in pairs for _ in range(2)],
        compiler_params=pltpu.CompilerParams(collective_id=0, has_side_effects=True),
    )(*args)


def solution(mesh):
    sp, tp = mesh.shape["sp"], mesh.shape["tp"]

    def program(*args):
        batch, span, features = args[0].shape
        rows, width = args[1].shape[1:]
        heads, head = args[4].shape[2:4]
        fits = (
            batch == 2
            and heads * batch == sp
            and heads == tp
            and head == rows
            and head % 128 == 0
            and heads * head == width
            and features == batch * rows
            and span % 16 == 0
        )
        return fused(batch, heads, tp, *args) if fits else body(*args)

    in_specs = (
        P(None, "sp", "tp"),
        P(None, "sp", "tp"),
        P(None, "sp", "tp"),
        P(None, "tp", "sp"),
        P(None, None, "tp", None, None),
        P(None, None, "tp", None, None),
        P(None, None, "tp"),
        P(None, None, "tp"),
        P(),
    )
    out_specs = P(None, "sp", "tp")
    return jax.shard_map(
        program, mesh=mesh, in_specs=in_specs, out_specs=out_specs, check_vma=False
    )
```
